32 devices in a mesh: rep: 2 (over x), fs: 8 (over z, y), tp: 2 (over core).
Axes of the slice: x: 2, y: 2, z: 4, core: 2. Of those that a mesh axis runs over, the one named last changes fastest.
Arguments:
- inputs_next: bfloat16 [2048, 2048], P(('rep', 'fs'), 'tp'), parts along dimension 0, may hold values from -6 to 6
- inputs_prev: bfloat16 [2048, 2048], P(('rep', 'fs'), 'tp'), parts along dimension 0, may hold values from -6 to 6
- hidden_prev: bfloat16 [2048, 8192], P(('rep', 'fs')), parts along dimension 0, may hold values from -6 to 6
- cotangent: bfloat16 [2048, 2048], P(('rep', 'fs'), 'tp'), parts along dimension 0, may hold values from -6 to 6
- up_weight: bfloat16 [2048, 8192], P('tp', 'fs'), may hold values from -0.125 to 0.125
- down_weight: bfloat16 [8192, 2048], P('fs', 'tp'), may hold values from -0.0625 to 0.0625
- up_accum: float32 [4096, 8192], P(('rep', 'tp'), 'fs'), parts along dimension 0, may hold values from -192 to 192
- down_accum: float32 [16384, 2048], P(('rep', 'fs'), 'tp'), parts along dimension 0, may hold values from -192 to 192
Outputs:
- output_next: bfloat16 [2048, 2048], P(('rep', 'fs'), 'tp'), parts along dimension 0
- hidden_next: bfloat16 [2048, 8192], P(('rep', 'fs')), parts along dimension 0
- input_grad: bfloat16 [2048, 2048], P(('rep', 'fs'), 'tp'), parts along dimension 0
- up_accum_out: float32 [4096, 8192], P(('rep', 'tp'), 'fs'), parts along dimension 0
- down_accum_out: float32 [16384, 2048], P(('rep', 'fs'), 'tp'), parts along dimension 0
The draws below stay inside these ranges and needn't reach their ends.
There are 2 independent parts, one for each index of `rep`. The reference program is written for one: setup_inputs(seed, part) draws one part's arguments, and reference() takes and returns one part's arrays. A program takes and returns all parts, laid end to end along the dimension named above; an argument that names none is the same for every part. Nothing has to cross between parts.
All inputs are finite; a program needn't handle non-finite values.
Results may differ from the reference program's by a relative error of at most 0.034.
Values may be sent and summed in bfloat16 or wider, within the bound.
A program may use at most 128 MiB of HBM per device.

```python
import jax
import jax.numpy as jnp

D = 2048
FF = 8192
TOKENS = 1024
N_TP = 2


def with_spikes(drawn, rng, source, target, blocks, factor):
    owner, partner = [(jnp.arange(drawn.shape[axis_at]) // (drawn.shape[axis_at] // blocks)).reshape([-1 if axis == axis_at else 1 for axis in range(drawn.ndim)]) for axis_at in (source, target)]
    chosen = jax.random.permutation(rng, blocks)[partner]
    strong = (owner == chosen) | (owner == (partner + blocks // 2) % blocks)
    return jnp.where(strong, factor * drawn, drawn)


def level_of(rng, dims, shards, low, largest):
    loudness = 1.0
    for position, shards_of in shards:
        heights = jax.random.uniform(jax.random.fold_in(jax.random.fold_in(rng, 6), position), (shards_of,), jnp.float32, low / len(shards), largest / len(shards))
        loudness = loudness * jnp.repeat(jnp.exp(heights), dims[position] // shards_of).reshape((-1,) + (1,) * (len(dims) - 1 - position))
    return loudness


def centred(own_key, dims, scale, most, split=(), held_as=jnp.bfloat16):
    level = level_of(own_key, dims, split, -0.22, 0.18) if split else 1.0
    values = jax.random.normal(own_key, dims, jnp.float32) * scale * level
    return jnp.minimum(jnp.maximum(values, -most), most).astype(held_as)


def heavy_noise(key, shape, deviation, reach, pieces, heavy, kind=jnp.bfloat16):
    drawn = deviation * jax.random.normal(key, shape, jnp.float32)
    if pieces:
        drawn = drawn * level_of(key, shape, pieces, -0.22, 0.18)
    return jnp.clip(with_spikes(drawn, jax.random.fold_in(key, 3), *heavy), -reach, reach).astype(kind)


def setup_inputs(seed: int = 0, part: int = 0) -> dict:
    splits = jax.random.split(jax.random.key(seed), 9)
    part_splits = jax.random.split(jax.random.fold_in(splits[8], part), 9)
    inputs_next = centred(part_splits[0], (TOKENS, D), 1.0, 6.0, ((0, 8), (1, 2)))
    inputs_prev = centred(part_splits[1], (TOKENS, D), 1.0, 6.0, ((0, 8), (1, 2)))
    hidden_prev = centred(part_splits[2], (TOKENS, FF), 1.0, 6.0, ((0, 8),))
    cotangent = heavy_noise(part_splits[3], (TOKENS, D), 1.0, 6.0, ((0, 8), (1, 2)), (0, 1, 8, 2.0))
    up_weight = centred(splits[4], (D, FF), D ** -0.5, 0.125, ((0, 2), (1, 8)))
    down_weight = centred(splits[5], (FF, D), FF ** -0.5, 0.0625, ((0, 8), (1, 2)))
    up_accum = centred(part_splits[6], (D, FF), 32.0, 192.0, ((0, 2), (1, 8)), jnp.float32)
    down_accum = centred(part_splits[7], (FF, D), 32.0, 192.0, ((0, 8), (1, 2)), jnp.float32)
    return {"inputs_next": inputs_next, "inputs_prev": inputs_prev, "hidden_prev": hidden_prev, "cotangent": cotangent, "up_weight": up_weight, "down_weight": down_weight, "up_accum": up_accum, "down_accum": down_accum}


def squared_relu(values):
    return jnp.square(jax.nn.relu(values.astype(jnp.float32))).astype(jnp.bfloat16)


def reference(inputs_next, inputs_prev, hidden_prev, cotangent, up_weight, down_weight, up_accum, down_accum):
    col_width = D // N_TP
    row_total = inputs_next.shape[0]
    hidden_total = jnp.zeros((row_total, FF), jnp.float32)
    back_total = jnp.zeros((row_total, FF), jnp.float32)
    for block_index in range(N_TP):
        start_col = block_index * col_width
        partial_value = jnp.dot(inputs_next[:, start_col:start_col + col_width], up_weight[start_col:start_col + col_width, :], preferred_element_type=jnp.float32)
        hidden_total = hidden_total + partial_value.astype(jnp.bfloat16).astype(jnp.float32)
        backward = jnp.dot(cotangent[:, start_col:start_col + col_width], down_weight[:, start_col:start_col + col_width].T, preferred_element_type=jnp.float32)
        back_total = back_total + backward.astype(jnp.bfloat16).astype(jnp.float32)
    hidden_next = hidden_total.astype(jnp.bfloat16)
    acts_next = squared_relu(hidden_next)
    output_next = jnp.dot(acts_next, down_weight, preferred_element_type=jnp.float32).astype(jnp.bfloat16)
    hidden_saved = hidden_prev.astype(jnp.float32)
    acts_prev = squared_relu(hidden_prev)
    hidden_grad = (back_total * 2.0 * jax.nn.relu(hidden_saved)).astype(jnp.bfloat16)
    input_grad = jnp.dot(hidden_grad, up_weight.T, preferred_element_type=jnp.float32).astype(jnp.bfloat16)
    up_accum_out = up_accum + jnp.dot(inputs_prev.T, hidden_grad, preferred_element_type=jnp.float32)
    down_accum_out = down_accum + jnp.dot(acts_prev.T, cotangent, preferred_element_type=jnp.float32)
    return (output_next, hidden_next, input_grad, up_accum_out, down_accum_out)
```

```python
import functools

import jax
import jax.numpy as jnp
from jax import lax
from jax.experimental import pallas as pl
from jax.experimental.pallas import tpu as pltpu
from jax.sharding import PartitionSpec as P

F32, BF16 = jnp.float32, jnp.bfloat16
PAIR = 2


def relu_squared(values):
    return jnp.square(jnp.maximum(values.astype(F32), 0.0)).astype(BF16)


def contract(left, right, left_dim, right_dim):
    return lax.dot_general(
        left, right, (((left_dim,), (right_dim,)), ((), ())), preferred_element_type=F32
    )


def send(src, dst, send_sem, recv_sem, **target):
    return pltpu.make_async_remote_copy(
        src_ref=src, dst_ref=dst, send_sem=send_sem, recv_sem=recv_sem,
        device_id=target, device_id_type=pl.DeviceIdType.MESH,
    )


def kernel(
    n_fs, n_tp, n_up, n_down,
    xn, xp, hp, ct, uw, dw, ua_hbm, da_hbm,
    out, hn, ig, uo_hbm, do_hbm,
    x_all, c_all, p_all, hp_all, h_all, hg_all,
    ht, bt, tp_h, tp_b, ot, it, ry_o, ry_i, ps_o, ps_i, rz_o, rz_i, ua, da,
    x_s, x_r, c_s, c_r, p_s, p_r, hps_s, hps_r, hpt_s, hpt_r,
    th_s, th_r, tb_s, tb_r, ah_s, ah_r, ab_s, ab_r, hna_s, hna_r, hnt_s, hnt_r,
    yo_s, yo_r, zo_s, zo_r, yi_s, yi_r, zi_s, zi_r, load_s, up_s, down_s,
):
    f, t = lax.axis_index("fs"), lax.axis_index("tp")
    n_z = n_fs // PAIR
    z, y = f // PAIR, lax.rem(f, PAIR)
    mate = z * PAIR + (1 - y)
    rows, width = xn.shape[0], dw.shape[0]
    part = rows // n_tp
    mine = pl.ds(pl.multiple_of(t * part, part), part)

    def z_peer(k):
        return lax.rem(z + k, n_z)

    def fs_peer(k):
        return lax.rem(f + k, n_fs)

    def tp_peer(k):
        return lax.rem(t + k, n_tp)

    def part_of(p):
        return pl.ds(pl.multiple_of(p * part, part), part)

    def unit(g):
        return pl.ds(pl.multiple_of(g * width, width), width)

    sent = []

    def go(copy):
        copy.start()
        sent.append(copy)

    def landed(dst, send_sem, recv_sem, **target):
        send(dst, dst, send_sem, recv_sem, **target).wait_recv()

    def gather_start(own, whole, ss, rs):
        for k in range(1, n_z):
            go(send(own, whole.at[f], ss.at[k], rs.at[f], fs=z_peer(k) * PAIR + y))
        go(send(own, whole.at[f], ss.at[0], rs.at[f], fs=mate))

    def gather_forward(own, whole, ss, rs):
        whole[f] = own[...]
        for k in range(1, n_z):
            src = z_peer(k) * PAIR + y
            landed(whole.at[src], ss.at[0], rs.at[src], fs=mate)
            go(send(whole.at[src], whole.at[src], ss.at[n_z + k - 1], rs.at[src], fs=mate))

    def gather_finish(whole, ss, rs):
        for k in range(n_z):
            src = z_peer(k) * PAIR + (1 - y)
            landed(whole.at[src], ss.at[0], rs.at[src], fs=mate)

    def tp_scatter(terms, held, ss, rs):
        for k in range(1, n_tp):
            p = tp_peer(k)
            go(send(terms.at[:, part_of(p), :], held.at[t], ss.at[k], rs.at[t], tp=p))

    def tp_scatter_wait(held, ss, rs):
        for k in range(1, n_tp):
            p = tp_peer(k)
            landed(held.at[p], ss.at[0], rs.at[p], tp=p)

    def tp_gather(view, ss, rs):
        for k in range(1, n_tp):
            go(send(view(mine), view(mine), ss.at[k], rs.at[t], tp=tp_peer(k)))

    def tp_gather_wait(view, ss, rs):
        for k in range(1, n_tp):
            p = tp_peer(k)
            landed(view(part_of(p)), ss.at[0], rs.at[p], tp=p)

    def tp_total(terms, held, i):
        total = terms[i, mine, :].astype(F32)
        for k in range(1, n_tp):
            total = total + held[tp_peer(k), i].astype(F32)
        return total

    def products(left_of, right, right_dim, terms):
        @pl.loop(0, n_fs // PAIR)
        def _(i):
            left = left_of(pl.ds(i * PAIR, PAIR))
            left = left.reshape(PAIR * rows, left.shape[-1])
            total = contract(left, right[...], 1, right_dim).astype(BF16)
            terms[pl.ds(i * PAIR, PAIR)] = total.reshape(PAIR, rows, total.shape[-1])

    def scatter_start(terms, ry, ss, rs):
        for k in range(n_z):
            zz = z_peer((k + 1) % n_z)
            go(send(terms.at[zz * PAIR + (1 - y)], ry.at[zz], ss.at[k], rs.at[zz], fs=mate))

    def scatter_pass(terms, ry, ps, rz, ss, rs, zs, zr):
        for k in range(1, n_z):
            zz = z_peer(k)
            landed(ry.at[zz], ss.at[0], rs.at[zz], fs=mate)
            ps[zz] = (terms[zz * PAIR + y].astype(F32) + ry[zz].astype(F32)).astype(BF16)
            go(send(ps.at[zz], rz.at[z], zs.at[k], zr.at[z], fs=zz * PAIR + y))

    def scatter_finish(terms, ry, rz, ss, rs, zs, zr, result):
        landed(ry.at[z], ss.at[0], rs.at[z], fs=mate)
        total = terms[f].astype(F32) + ry[z].astype(F32)
        for k in range(1, n_z):
            zz = z_peer(k)
            landed(rz.at[zz], zs.at[0], zr.at[zz], fs=zz * PAIR + y)
            total = total + rz[zz].astype(F32)
        result[...] = total.astype(BF16)

    barrier = pltpu.get_barrier_semaphore()
    for k in range(1, n_fs):
        pl.semaphore_signal(
            barrier, inc=1, device_id={"fs": fs_peer(k)}, device_id_type=pl.DeviceIdType.MESH
        )
    for k in range(1, n_tp):
        pl.semaphore_signal(
            barrier, inc=1, device_id={"tp": tp_peer(k)}, device_id_type=pl.DeviceIdType.MESH
        )
    pl.semaphore_wait(barrier, n_fs + n_tp - 2)

    gather_start(xn, x_all, x_s, x_r)
    gather_start(ct, c_all, c_s, c_r)
    for k in range(1, n_fs):
        g = fs_peer(k)
        go(send(hp.at[mine, unit(g)], hp_all.at[f, mine, :], hps_s.at[k], hps_r.at[f], fs=g))
    loads = [
        pltpu.make_async_copy(ua_hbm, ua, load_s.at[0]),
        pltpu.make_async_copy(da_hbm, da, load_s.at[1]),
    ]
    for load in loads:
        load.start()
    hp_all[f, mine, :] = hp[mine, unit(f)]

    gather_forward(xn, x_all, x_s, x_r)
    gather_finish(x_all, x_s, x_r)
    products(lambda at: x_all[at], uw, 0, ht)
    tp_scatter(ht, tp_h, th_s, th_r)
    tp_scatter_wait(tp_h, th_s, th_r)

    @pl.loop(0, n_fs)
    def _(i):
        h_all[i, mine, :] = tp_total(ht, tp_h, i).astype(BF16)

    tp_gather(lambda at: h_all.at[:, at, :], ah_s, ah_r)
    for k in range(1, n_fs):
        g = fs_peer(k)
        go(send(h_all.at[g, mine, :], hn.at[mine, unit(f)], hna_s.at[k], hna_r.at[f], fs=g))
    hn[mine, unit(f)] = h_all[f, mine, :]
    tp_gather_wait(lambda at: h_all.at[:, at, :], ah_s, ah_r)
    products(lambda at: relu_squared(h_all[at]), dw, 0, ot)
    scatter_start(ot, ry_o, yo_s, yo_r)

    gather_forward(ct, c_all, c_s, c_r)
    gather_start(xp, p_all, p_s, p_r)
    scatter_pass(ot, ry_o, ps_o, rz_o, yo_s, yo_r, zo_s, zo_r)
    gather_finish(c_all, c_s, c_r)
    products(lambda at: c_all[at], dw, 1, bt)
    tp_scatter(bt, tp_b, tb_s, tb_r)
    for k in range(1, n_fs):
        g = fs_peer(k)
        landed(hp_all.at[g, mine, :], hps_s.at[0], hps_r.at[g], fs=g)
    tp_gather(lambda at: hp_all.at[:, at, :], hpt_s, hpt_r)
    tp_scatter_wait(tp_b, tb_s, tb_r)

    @pl.loop(0, n_fs)
    def _(i):
        slope = jnp.maximum(hp_all[i, mine, :].astype(F32), 0.0)
        hg_all[i, mine, :] = (tp_total(bt, tp_b, i) * 2.0 * slope).astype(BF16)

    tp_gather(lambda at: hg_all.at[:, at, :], ab_s, ab_r)
    tp_gather_wait(lambda at: hg_all.at[:, at, :], ab_s, ab_r)
    products(lambda at: hg_all[at], uw, 1, it)
    scatter_start(it, ry_i, yi_s, yi_r)
    gather_forward(xp, p_all, p_s, p_r)

    tp_gather_wait(lambda at: hp_all.at[:, at, :], hpt_s, hpt_r)
    for load in loads:
        load.wait()

    def accumulate(left_of, right, total, hbm, sems, pieces):
        high = total.shape[0] // pieces

        def piece(i):
            return pl.ds(pl.multiple_of(i * high, high), high)

        @pl.loop(0, pieces)
        def _(i):
            left = left_of(piece(i)).reshape(n_fs * rows, high)
            flat = right[...].reshape(n_fs * rows, right.shape[-1])
            total[piece(i), :] += contract(left, flat, 0, 0)
            pltpu.make_async_copy(total.at[piece(i), :], hbm.at[piece(i), :], sems.at[i]).start()

        def drain():
            for i in range(pieces):
                at = pl.ds(i * high, high)
                pltpu.make_async_copy(total.at[at, :], hbm.at[at, :], sems.at[i]).wait()

        return drain

    drain_down = accumulate(
        lambda at: relu_squared(hp_all[:, :, at]), c_all, da, do_hbm, down_s, n_down
    )
    scatter_pass(it, ry_i, ps_i, rz_i, yi_s, yi_r, zi_s, zi_r)

    for k in range(1, n_fs):
        g = fs_peer(k)
        landed(hn.at[mine, unit(g)], hna_s.at[0], hna_r.at[g], fs=g)
    tp_gather(lambda at: hn.at[at, :], hnt_s, hnt_r)
    scatter_finish(ot, ry_o, rz_o, yo_s, yo_r, zo_s, zo_r, out)
    gather_finish(p_all, p_s, p_r)
    drain_up = accumulate(lambda at: p_all[:, :, at], hg_all, ua, uo_hbm, up_s, n_up)
    scatter_finish(it, ry_i, rz_i, yi_s, yi_r, zi_s, zi_r, ig)
    tp_gather_wait(lambda at: hn.at[at, :], hnt_s, hnt_r)
    drain_down()
    drain_up()
    for copy in sent:
        copy.wait_send()


def local(n_fs, n_tp, xn, xp, hp, ct, uw, dw, ua, da):
    rows, depth = xn.shape
    width = dw.shape[0]
    n_z = n_fs // PAIR
    part = rows // n_tp
    n_up, n_down = max(1, depth // 256), max(1, width // 256)
    dma = pltpu.SemaphoreType.DMA

    def held(*shape, dtype=BF16):
        return pltpu.VMEM(shape, dtype)

    def tokens(columns):
        return held(n_fs, rows, columns)

    vmem, anywhere = pl.BlockSpec(memory_space=pltpu.VMEM), pl.BlockSpec(memory_space=pl.ANY)
    fs_sem, tp_sem, z_sem = dma((n_fs,)), dma((n_tp,)), dma((n_z,))
    return pl.pallas_call(
        functools.partial(kernel, n_fs, n_tp, n_up, n_down),
        out_shape=(
            jax.ShapeDtypeStruct(xn.shape, BF16),
            jax.ShapeDtypeStruct(hp.shape, BF16),
            jax.ShapeDtypeStruct(xp.shape, BF16),
            jax.ShapeDtypeStruct(ua.shape, F32),
            jax.ShapeDtypeStruct(da.shape, F32),
        ),
        in_specs=[vmem] * 6 + [anywhere] * 2,
        out_specs=(vmem, vmem, vmem, anywhere, anywhere),
        scratch_shapes=[
            tokens(depth), tokens(depth), tokens(depth),
            tokens(width), tokens(width), tokens(width),
            tokens(width), tokens(width),
            held(n_tp, n_fs, part, width), held(n_tp, n_fs, part, width),
            tokens(depth), tokens(depth),
            held(n_z, rows, depth), held(n_z, rows, depth),
            held(n_z, rows, depth), held(n_z, rows, depth),
            held(n_z, rows, depth), held(n_z, rows, depth),
            held(*ua.shape, dtype=F32), held(*da.shape, dtype=F32),
            fs_sem, fs_sem, fs_sem, fs_sem, fs_sem, fs_sem, fs_sem, fs_sem, tp_sem, tp_sem,
            tp_sem, tp_sem, tp_sem, tp_sem, tp_sem, tp_sem, tp_sem, tp_sem,
            fs_sem, fs_sem, tp_sem, tp_sem,
            z_sem, z_sem, z_sem, z_sem, z_sem, z_sem, z_sem, z_sem,
            dma((2,)), dma((n_up,)), dma((n_down,)),
        ],
        compiler_params=pltpu.CompilerParams(
            collective_id=0, has_side_effects=True, vmem_limit_bytes=62 * 1024 * 1024
        ),
    )(xn, xp, hp, ct, uw, dw, ua, da)


def solution(mesh):
    return jax.shard_map(
        functools.partial(local, mesh.shape["fs"], mesh.shape["tp"]),
        mesh=mesh,
        in_specs=(
            P(("rep", "fs"), "tp"),
            P(("rep", "fs"), "tp"),
            P(("rep", "fs"), None),
            P(("rep", "fs"), "tp"),
            P("tp", "fs"),
            P("fs", "tp"),
            P(("rep", "tp"), "fs"),
            P(("rep", "fs"), "tp"),
        ),
        out_specs=(
            P(("rep", "fs"), "tp"),
            P(("rep", "fs"), None),
            P(("rep", "fs"), "tp"),
            P(("rep", "tp"), "fs"),
            P(("rep", "fs"), "tp"),
        ),
        check_vma=False,
    )
```

```python
import functools

import jax
import jax.numpy as jnp
from jax import lax
from jax.experimental import pallas as pl
from jax.experimental.pallas import tpu as pltpu
from jax.sharding import PartitionSpec as P

F32, BF16 = jnp.float32, jnp.bfloat16
PAIR = 2


def relu_squared(values):
    return jnp.square(jnp.maximum(values.astype(F32), 0.0)).astype(BF16)


def contract(left, right, left_dim, right_dim):
    return lax.dot_general(
        left, right, (((left_dim,), (right_dim,)), ((), ())), preferred_element_type=F32
    )


def send(src, dst, send_sem, recv_sem, **target):
    return pltpu.make_async_remote_copy(
        src_ref=src, dst_ref=dst, send_sem=send_sem, recv_sem=recv_sem,
        device_id=target, device_id_type=pl.DeviceIdType.MESH,
    )


def kernel(
    n_fs, n_tp, n_up, n_down,
    xn, xp, hp, ct, uw, dw, ua_hbm, da_hbm,
    out, hn, ig, uo_hbm, do_hbm,
    x_all, c_all, p_all, hp_all, h_all, hg_all,
    ht, bt, tp_h, tp_b, ot, it, ry_o, ry_i, ps_o, ps_i, rr_o, rr_i, rz_o, rz_i, ua, da,
    x_s, x_r, c_s, c_r, p_s, p_r, hps_s, hps_r, hpt_s, hpt_r,
    th_s, th_r, tb_s, tb_r, ah_s, ah_r, ab_s, ab_r, hna_s, hna_r, hnt_s, hnt_r,
    yo_s, yo_r, zo_s, zo_r, yi_s, yi_r, zi_s, zi_r, ro_s, ro_r, ri_s, ri_r, load_s, up_s, down_s,
):
    f, t = lax.axis_index("fs"), lax.axis_index("tp")
    n_z = n_fs // PAIR
    z, y = f // PAIR, lax.rem(f, PAIR)
    mate = z * PAIR + (1 - y)
    hs = n_z // 2
    low, at_half = z // hs * hs, lax.rem(z, hs)
    rows, width = xn.shape[0], dw.shape[0]
    part = rows // n_tp
    mine = pl.ds(pl.multiple_of(t * part, part), part)

    def z_peer(k):
        return lax.rem(z + k, n_z)

    def cross_of(zz):
        return lax.rem(zz + hs, n_z)

    cross = cross_of(z)

    def half_peer(k):
        return low + lax.rem(at_half + k, hs)

    def fs_peer(k):
        return lax.rem(f + k, n_fs)

    def tp_peer(k):
        return lax.rem(t + k, n_tp)

    def part_of(p):
        return pl.ds(pl.multiple_of(p * part, part), part)

    def unit(g):
        return pl.ds(pl.multiple_of(g * width, width), width)

    sent = []

    def go(copy):
        copy.start()
        sent.append(copy)

    def landed(dst, send_sem, recv_sem, **target):
        send(dst, dst, send_sem, recv_sem, **target).wait_recv()

    class Gather:
        def __init__(self, own, whole, ss, rs):
            self.own, self.whole, self.ss, self.rs, self.used = own, whole, ss, rs, 0

        def put(self, src, block, g):
            go(send(src, self.whole.at[block], self.ss.at[self.used], self.rs.at[block], fs=g))
            self.used += 1

        def wait(self, block):
            landed(self.whole.at[block], self.ss.at[0], self.rs.at[block], fs=mate)

        def start(self):
            self.put(self.own, f, cross * PAIR + y)
            for k in range(1, hs):
                self.put(self.own, f, half_peer(k) * PAIR + y)
            self.whole[f] = self.own[...]

        def start_mate(self):
            self.put(self.own, f, mate)

        def relay(self):
            block = cross * PAIR + y
            self.wait(block)
            for k in range(1, hs):
                self.put(self.whole.at[block], block, half_peer(k) * PAIR + y)
            self.put(self.whole.at[block], block, mate)

        def forward(self):
            for move in (lambda p: p, cross_of):
                for k in range(1, hs):
                    block = move(half_peer(k)) * PAIR + y
                    self.wait(block)
                    self.put(self.whole.at[block], block, mate)

        def finish(self):
            for k in range(n_z):
                self.wait(z_peer(k) * PAIR + (1 - y))

    def tp_scatter(terms, held, ss, rs):
        for k in range(1, n_tp):
            p = tp_peer(k)
            go(send(terms.at[:, part_of(p), :], held.at[t], ss.at[k], rs.at[t], tp=p))

    def tp_scatter_wait(held, ss, rs):
        for k in range(1, n_tp):
            p = tp_peer(k)
            landed(held.at[p], ss.at[0], rs.at[p], tp=p)

    def tp_gather(view, ss, rs):
        for k in range(1, n_tp):
            go(send(view(mine), view(mine), ss.at[k], rs.at[t], tp=tp_peer(k)))

    def tp_gather_wait(view, ss, rs):
        for k in range(1, n_tp):
            p = tp_peer(k)
            landed(view(part_of(p)), ss.at[0], rs.at[p], tp=p)

    def tp_total(terms, held, i):
        total = terms[i, mine, :].astype(F32)
        for k in range(1, n_tp):
            total = total + held[tp_peer(k), i].astype(F32)
        return total

    def products(left_of, right, right_dim, terms):
        @pl.loop(0, n_fs // PAIR)
        def _(i):
            left = left_of(pl.ds(i * PAIR, PAIR))
            left = left.reshape(PAIR * rows, left.shape[-1])
            total = contract(left, right[...], 1, right_dim).astype(BF16)
            terms[pl.ds(i * PAIR, PAIR)] = total.reshape(PAIR, rows, total.shape[-1])

    class Scatter:
        def __init__(self, terms, ry, ps, rr, rz, sems):
            self.terms, self.ry, self.ps, self.rr, self.rz = terms, ry, ps, rr, rz
            self.ys, self.yr, self.rs, self.rrecv, self.zs, self.zr = sems

        def start(self):
            order = [cross_of(half_peer(k)) for k in range(1, hs)] + [cross]
            order += [half_peer(k) for k in range(1, hs)] + [z]
            for k, zz in enumerate(order):
                block = self.terms.at[zz * PAIR + (1 - y)]
                go(send(block, self.ry.at[zz], self.ys.at[k], self.yr.at[zz], fs=mate))

        def pair(self, zz):
            landed(self.ry.at[zz], self.ys.at[0], self.yr.at[zz], fs=mate)
            return self.terms[zz * PAIR + y].astype(F32) + self.ry[zz].astype(F32)

        def spread(self):
            for k in range(1, hs):
                p = half_peer(k)
                zz = cross_of(p)
                self.ps[zz] = self.pair(zz).astype(BF16)
                slot, sem = self.rr.at[at_half], self.rrecv.at[at_half]
                go(send(self.ps.at[zz], slot, self.rs.at[k], sem, fs=p * PAIR + y))

        def relay(self):
            total = self.pair(cross)
            for k in range(1, hs):
                p = half_peer(k)
                w = p - low
                landed(self.rr.at[w], self.rs.at[0], self.rrecv.at[w], fs=p * PAIR + y)
                total = total + self.rr[w].astype(F32)
            self.ps[cross] = total.astype(BF16)
            go(send(
                self.ps.at[cross], self.rz.at[hs], self.zs.at[0], self.zr.at[hs],
                fs=cross * PAIR + y,
            ))
            for k in range(1, hs):
                p = half_peer(k)
                self.ps[p] = self.pair(p).astype(BF16)
                slot, sem = self.rz.at[at_half], self.zr.at[at_half]
                go(send(self.ps.at[p], slot, self.zs.at[k], sem, fs=p * PAIR + y))

        def finish(self, result):
            total = self.pair(z)
            for k in range(1, hs):
                p = half_peer(k)
                w = p - low
                landed(self.rz.at[w], self.zs.at[0], self.zr.at[w], fs=p * PAIR + y)
                total = total + self.rz[w].astype(F32)
            landed(self.rz.at[hs], self.zs.at[0], self.zr.at[hs], fs=cross * PAIR + y)
            result[...] = (total + self.rz[hs].astype(F32)).astype(BF16)

    barrier = pltpu.get_barrier_semaphore()
    for k in range(1, n_fs):
        pl.semaphore_signal(
            barrier, inc=1, device_id={"fs": fs_peer(k)}, device_id_type=pl.DeviceIdType.MESH
        )
    for k in range(1, n_tp):
        pl.semaphore_signal(
            barrier, inc=1, device_id={"tp": tp_peer(k)}, device_id_type=pl.DeviceIdType.MESH
        )
    pl.semaphore_wait(barrier, n_fs + n_tp - 2)

    gx = Gather(xn, x_all, x_s, x_r)
    gc = Gather(ct, c_all, c_s, c_r)
    gp = Gather(xp, p_all, p_s, p_r)
    sum_o = Scatter(ot, ry_o, ps_o, rr_o, rz_o, (yo_s, yo_r, ro_s, ro_r, zo_s, zo_r))
    sum_i = Scatter(it, ry_i, ps_i, rr_i, rz_i, (yi_s, yi_r, ri_s, ri_r, zi_s, zi_r))

    gx.start()
    gx.start_mate()
    loads = [
        pltpu.make_async_copy(ua_hbm, ua, load_s.at[0]),
        pltpu.make_async_copy(da_hbm, da, load_s.at[1]),
    ]
    for load in loads:
        load.start()
    hp_all[f, mine, :] = hp[mine, unit(f)]
    gx.relay()
    gc.start()
    gx.forward()
    gc.start_mate()
    gc.relay()
    for k in range(1, n_fs):
        g = fs_peer(k)
        go(send(hp.at[mine, unit(g)], hp_all.at[f, mine, :], hps_s.at[k], hps_r.at[f], fs=g))

    gx.finish()
    products(lambda at: x_all[at], uw, 0, ht)
    tp_scatter(ht, tp_h, th_s, th_r)
    gc.forward()
    tp_scatter_wait(tp_h, th_s, th_r)

    @pl.loop(0, n_fs)
    def _(i):
        h_all[i, mine, :] = tp_total(ht, tp_h, i).astype(BF16)

    tp_gather(lambda at: h_all.at[:, at, :], ah_s, ah_r)
    for k in range(1, n_fs):
        g = fs_peer(k)
        go(send(h_all.at[g, mine, :], hn.at[mine, unit(f)], hna_s.at[k], hna_r.at[f], fs=g))
    hn[mine, unit(f)] = h_all[f, mine, :]
    tp_gather_wait(lambda at: h_all.at[:, at, :], ah_s, ah_r)
    products(lambda at: relu_squared(h_all[at]), dw, 0, ot)
    sum_o.start()
    gp.start()

    gc.finish()
    products(lambda at: c_all[at], dw, 1, bt)
    tp_scatter(bt, tp_b, tb_s, tb_r)
    for k in range(1, n_fs):
        g = fs_peer(k)
        landed(hp_all.at[g, mine, :], hps_s.at[0], hps_r.at[g], fs=g)
    tp_gather(lambda at: hp_all.at[:, at, :], hpt_s, hpt_r)
    tp_scatter_wait(tp_b, tb_s, tb_r)

    @pl.loop(0, n_fs)
    def _(i):
        slope = jnp.maximum(hp_all[i, mine, :].astype(F32), 0.0)
        hg_all[i, mine, :] = (tp_total(bt, tp_b, i) * 2.0 * slope).astype(BF16)

    tp_gather(lambda at: hg_all.at[:, at, :], ab_s, ab_r)
    tp_gather_wait(lambda at: hg_all.at[:, at, :], ab_s, ab_r)
    products(lambda at: hg_all[at], uw, 1, it)
    sum_i.start()
    sum_o.spread()
    sum_o.relay()
    gp.start_mate()
    gp.relay()
    gp.forward()

    tp_gather_wait(lambda at: hp_all.at[:, at, :], hpt_s, hpt_r)
    for load in loads:
        load.wait()

    def accumulate(left_of, right, total, hbm, sems, pieces):
        high = total.shape[0] // pieces

        def piece(i):
            return pl.ds(pl.multiple_of(i * high, high), high)

        @pl.loop(0, pieces)
        def _(i):
            left = left_of(piece(i)).reshape(n_fs * rows, high)
            flat = right[...].reshape(n_fs * rows, right.shape[-1])
            total[piece(i), :] += contract(left, flat, 0, 0)
            pltpu.make_async_copy(total.at[piece(i), :], hbm.at[piece(i), :], sems.at[i]).start()

        def drain():
            for i in range(pieces):
                at = pl.ds(i * high, high)
                pltpu.make_async_copy(total.at[at, :], hbm.at[at, :], sems.at[i]).wait()

        return drain

    drain_down = accumulate(
        lambda at: relu_squared(hp_all[:, :, at]), c_all, da, do_hbm, down_s, n_down
    )
    sum_i.spread()
    sum_i.relay()

    for k in range(1, n_fs):
        g = fs_peer(k)
        landed(hn.at[mine, unit(g)], hna_s.at[0], hna_r.at[g], fs=g)
    tp_gather(lambda at: hn.at[at, :], hnt_s, hnt_r)
    sum_o.finish(out)
    gp.finish()
    drain_up = accumulate(lambda at: p_all[:, :, at], hg_all, ua, uo_hbm, up_s, n_up)
    sum_i.finish(ig)
    tp_gather_wait(lambda at: hn.at[at, :], hnt_s, hnt_r)
    drain_down()
    drain_up()
    for copy in sent:
        copy.wait_send()


def local(n_fs, n_tp, xn, xp, hp, ct, uw, dw, ua, da):
    rows, depth = xn.shape
    width = dw.shape[0]
    n_z = n_fs // PAIR
    part = rows // n_tp
    n_up, n_down = max(1, depth // 256), max(1, width // 256)
    dma = pltpu.SemaphoreType.DMA

    def held(*shape, dtype=BF16):
        return pltpu.VMEM(shape, dtype)

    def tokens(columns):
        return held(n_fs, rows, columns)

    vmem, anywhere = pl.BlockSpec(memory_space=pltpu.VMEM), pl.BlockSpec(memory_space=pl.ANY)
    fs_sem, tp_sem, z_sem = dma((n_fs,)), dma((n_tp,)), dma((n_z,))
    return pl.pallas_call(
        functools.partial(kernel, n_fs, n_tp, n_up, n_down),
        out_shape=(
            jax.ShapeDtypeStruct(xn.shape, BF16),
            jax.ShapeDtypeStruct(hp.shape, BF16),
            jax.ShapeDtypeStruct(xp.shape, BF16),
            jax.ShapeDtypeStruct(ua.shape, F32),
            jax.ShapeDtypeStruct(da.shape, F32),
        ),
        in_specs=[vmem] * 6 + [anywhere] * 2,
        out_specs=(vmem, vmem, vmem, anywhere, anywhere),
        scratch_shapes=[
            tokens(depth), tokens(depth), tokens(depth),
            tokens(width), tokens(width), tokens(width),
            tokens(width), tokens(width),
            held(n_tp, n_fs, part, width), held(n_tp, n_fs, part, width),
            tokens(depth), tokens(depth),
            held(n_z, rows, depth), held(n_z, rows, depth),
            held(n_z, rows, depth), held(n_z, rows, depth),
            held(n_z // 2, rows, depth), held(n_z // 2, rows, depth),
            held(n_z // 2 + 1, rows, depth), held(n_z // 2 + 1, rows, depth),
            held(*ua.shape, dtype=F32), held(*da.shape, dtype=F32),
            fs_sem, fs_sem, fs_sem, fs_sem, fs_sem, fs_sem, fs_sem, fs_sem, tp_sem, tp_sem,
            tp_sem, tp_sem, tp_sem, tp_sem, tp_sem, tp_sem, tp_sem, tp_sem,
            fs_sem, fs_sem, tp_sem, tp_sem,
            z_sem, z_sem, z_sem, z_sem, z_sem, z_sem, z_sem, z_sem,
            z_sem, z_sem, z_sem, z_sem,
            dma((2,)), dma((n_up,)), dma((n_down,)),
        ],
        compiler_params=pltpu.CompilerParams(
            collective_id=0, has_side_effects=True, vmem_limit_bytes=62 * 1024 * 1024
        ),
    )(xn, xp, hp, ct, uw, dw, ua, da)


def solution(mesh):
    return jax.shard_map(
        functools.partial(local, mesh.shape["fs"], mesh.shape["tp"]),
        mesh=mesh,
        in_specs=(
            P(("rep", "fs"), "tp"),
            P(("rep", "fs"), "tp"),
            P(("rep", "fs"), None),
            P(("rep", "fs"), "tp"),
            P("tp", "fs"),
            P("fs", "tp"),
            P(("rep", "tp"), "fs"),
            P(("rep", "fs"), "tp"),
        ),
        out_specs=(
            P(("rep", "fs"), "tp"),
            P(("rep", "fs"), None),
            P(("rep", "fs"), "tp"),
            P(("rep", "tp"), "fs"),
            P(("rep", "fs"), "tp"),
        ),
        check_vma=False,
    )
```

```python
import functools

import jax
import jax.numpy as jnp
from jax import lax
from jax.experimental import pallas as pl
from jax.experimental.pallas import tpu as pltpu
from jax.sharding import PartitionSpec as P

F32, BF16 = jnp.float32, jnp.bfloat16
PAIR = 2


def relu_squared(values):
    return jnp.square(jnp.maximum(values.astype(F32), 0.0)).astype(BF16)


def contract(left, right, left_dim, right_dim):
    return lax.dot_general(
        left, right, (((left_dim,), (right_dim,)), ((), ())), preferred_element_type=F32
    )


def send(src, dst, send_sem, recv_sem, **target):
    return pltpu.make_async_remote_copy(
        src_ref=src, dst_ref=dst, send_sem=send_sem, recv_sem=recv_sem,
        device_id=target, device_id_type=pl.DeviceIdType.MESH,
    )


def kernel(
    n_fs, n_tp,
    xn_hbm, xp_hbm, hp_hbm, ct_hbm, uw_hbm, dw_hbm, ua_hbm, da_hbm,
    out, hn, ig, ua, da,
    xn, xp, hp, ct, uw, dw,
    x_all, c_all, p_all, hp_all, h_all, hg_all,
    ht, bt, tp_h, tp_b, ot, it, ry_o, ry_i, ps_o, ps_i, rr_o, rr_i, rz_o, rz_i,
    x_s, x_r, c_s, c_r, p_s, p_r, hps_s, hps_r, hpt_s, hpt_r,
    th_s, th_r, tb_s, tb_r, ah_s, ah_r, ab_s, ab_r, hna_s, hna_r, hnt_s, hnt_r,
    yo_s, yo_r, zo_s, zo_r, yi_s, yi_r, zi_s, zi_r, ro_s, ro_r, ri_s, ri_r, load_s,
):
    f, t = lax.axis_index("fs"), lax.axis_index("tp")
    n_z = n_fs // PAIR
    z, y = f // PAIR, lax.rem(f, PAIR)
    mate = z * PAIR + (1 - y)
    hs = n_z // 2
    low, at_half = z // hs * hs, lax.rem(z, hs)
    rows, width = xn.shape[0], dw.shape[0]
    part = rows // n_tp
    mine = pl.ds(pl.multiple_of(t * part, part), part)

    def z_peer(k):
        return lax.rem(z + k, n_z)

    def cross_of(zz):
        return lax.rem(zz + hs, n_z)

    cross = cross_of(z)

    def half_peer(k):
        return low + lax.rem(at_half + k, hs)

    def fs_peer(k):
        return lax.rem(f + k, n_fs)

    def tp_peer(k):
        return lax.rem(t + k, n_tp)

    def part_of(p):
        return pl.ds(pl.multiple_of(p * part, part), part)

    def unit(g):
        return pl.ds(pl.multiple_of(g * width, width), width)

    sent = []

    def go(copy):
        copy.start()
        sent.append(copy)

    def landed(dst, send_sem, recv_sem, **target):
        send(dst, dst, send_sem, recv_sem, **target).wait_recv()

    class Gather:
        def __init__(self, own, whole, ss, rs):
            self.own, self.whole, self.ss, self.rs, self.used = own, whole, ss, rs, 0

        def put(self, src, block, g):
            go(send(src, self.whole.at[block], self.ss.at[self.used], self.rs.at[block], fs=g))
            self.used += 1

        def wait(self, block):
            landed(self.whole.at[block], self.ss.at[0], self.rs.at[block], fs=mate)

        def start(self):
            self.put(self.own, f, cross * PAIR + y)
            for k in range(1, hs):
                self.put(self.own, f, half_peer(k) * PAIR + y)
            self.whole[f] = self.own[...]

        def start_mate(self):
            self.put(self.own, f, mate)

        def relay(self):
            block = cross * PAIR + y
            self.wait(block)
            for k in range(1, hs):
                self.put(self.whole.at[block], block, half_peer(k) * PAIR + y)
            self.put(self.whole.at[block], block, mate)

        def forward(self):
            for move in (lambda p: p, cross_of):
                for k in range(1, hs):
                    block = move(half_peer(k)) * PAIR + y
                    self.wait(block)
                    self.put(self.whole.at[block], block, mate)

        def finish(self):
            for k in range(n_z):
                self.wait(z_peer(k) * PAIR + (1 - y))

    def tp_scatter(terms, held, ss, rs):
        for k in range(1, n_tp):
            p = tp_peer(k)
            go(send(terms.at[:, part_of(p), :], held.at[t], ss.at[k], rs.at[t], tp=p))

    def tp_scatter_wait(held, ss, rs):
        for k in range(1, n_tp):
            p = tp_peer(k)
            landed(held.at[p], ss.at[0], rs.at[p], tp=p)

    def tp_gather(view, ss, rs):
        for k in range(1, n_tp):
            go(send(view(mine), view(mine), ss.at[k], rs.at[t], tp=tp_peer(k)))

    def tp_gather_wait(view, ss, rs):
        for k in range(1, n_tp):
            p = tp_peer(k)
            landed(view(part_of(p)), ss.at[0], rs.at[p], tp=p)

    def tp_total(terms, held, i):
        total = terms[i, mine, :].astype(F32)
        for k in range(1, n_tp):
            total = total + held[tp_peer(k), i].astype(F32)
        return total

    def products(left_of, right, right_dim, terms):
        @pl.loop(0, n_fs // PAIR)
        def _(i):
            left = left_of(pl.ds(i * PAIR, PAIR))
            left = left.reshape(PAIR * rows, left.shape[-1])
            total = contract(left, right[...], 1, right_dim).astype(BF16)
            terms[pl.ds(i * PAIR, PAIR)] = total.reshape(PAIR, rows, total.shape[-1])

    class Scatter:
        def __init__(self, terms, ry, ps, rr, rz, sems):
            self.terms, self.ry, self.ps, self.rr, self.rz = terms, ry, ps, rr, rz
            self.ys, self.yr, self.rs, self.rrecv, self.zs, self.zr = sems

        def start(self):
            order = [cross_of(half_peer(k)) for k in range(1, hs)] + [cross]
            order += [half_peer(k) for k in range(1, hs)] + [z]
            for k, zz in enumerate(order):
                block = self.terms.at[zz * PAIR + (1 - y)]
                go(send(block, self.ry.at[zz], self.ys.at[k], self.yr.at[zz], fs=mate))

        def pair(self, zz):
            landed(self.ry.at[zz], self.ys.at[0], self.yr.at[zz], fs=mate)
            return self.terms[zz * PAIR + y].astype(F32) + self.ry[zz].astype(F32)

        def spread(self):
            for k in range(1, hs):
                p = half_peer(k)
                zz = cross_of(p)
                self.ps[zz] = self.pair(zz).astype(BF16)
                slot, sem = self.rr.at[at_half], self.rrecv.at[at_half]
                go(send(self.ps.at[zz], slot, self.rs.at[k], sem, fs=p * PAIR + y))

        def relay(self):
            total = self.pair(cross)
            for k in range(1, hs):
                p = half_peer(k)
                w = p - low
                landed(self.rr.at[w], self.rs.at[0], self.rrecv.at[w], fs=p * PAIR + y)
                total = total + self.rr[w].astype(F32)
            self.ps[cross] = total.astype(BF16)
            go(send(
                self.ps.at[cross], self.rz.at[hs], self.zs.at[0], self.zr.at[hs],
                fs=cross * PAIR + y,
            ))
            for k in range(1, hs):
                p = half_peer(k)
                self.ps[p] = self.pair(p).astype(BF16)
                slot, sem = self.rz.at[at_half], self.zr.at[at_half]
                go(send(self.ps.at[p], slot, self.zs.at[k], sem, fs=p * PAIR + y))

        def finish(self, result):
            total = self.pair(z)
            for k in range(1, hs):
                p = half_peer(k)
                w = p - low
                landed(self.rz.at[w], self.zs.at[0], self.zr.at[w], fs=p * PAIR + y)
                total = total + self.rz[w].astype(F32)
            landed(self.rz.at[hs], self.zs.at[0], self.zr.at[hs], fs=cross * PAIR + y)
            result[...] = (total + self.rz[hs].astype(F32)).astype(BF16)

    def load(k, src, dst):
        copy = pltpu.make_async_copy(src, dst, load_s.at[k])
        copy.start()
        return copy

    load_xn, load_ct, load_xp = load(0, xn_hbm, xn), load(1, ct_hbm, ct), load(2, xp_hbm, xp)
    load_hp, load_uw, load_dw = load(3, hp_hbm, hp), load(4, uw_hbm, uw), load(5, dw_hbm, dw)
    load_ua, load_da = load(6, ua_hbm, ua), load(7, da_hbm, da)

    barrier = pltpu.get_barrier_semaphore()
    for k in range(1, n_fs):
        pl.semaphore_signal(
            barrier, inc=1, device_id={"fs": fs_peer(k)}, device_id_type=pl.DeviceIdType.MESH
        )
    for k in range(1, n_tp):
        pl.semaphore_signal(
            barrier, inc=1, device_id={"tp": tp_peer(k)}, device_id_type=pl.DeviceIdType.MESH
        )
    pl.semaphore_wait(barrier, n_fs + n_tp - 2)

    gx = Gather(xn, x_all, x_s, x_r)
    gc = Gather(ct, c_all, c_s, c_r)
    gp = Gather(xp, p_all, p_s, p_r)
    sum_o = Scatter(ot, ry_o, ps_o, rr_o, rz_o, (yo_s, yo_r, ro_s, ro_r, zo_s, zo_r))
    sum_i = Scatter(it, ry_i, ps_i, rr_i, rz_i, (yi_s, yi_r, ri_s, ri_r, zi_s, zi_r))

    load_xn.wait()
    gx.start()
    gx.start_mate()
    load_ct.wait()
    gc.start_mate()
    load_xp.wait()
    load_hp.wait()
    hp_all[f, mine, :] = hp[mine, unit(f)]
    load_uw.wait()
    load_dw.wait()
    gx.relay()
    gc.start()
    gx.forward()
    gc.relay()
    for k in range(1, n_fs):
        g = fs_peer(k)
        go(send(hp.at[mine, unit(g)], hp_all.at[f, mine, :], hps_s.at[k], hps_r.at[f], fs=g))

    gx.finish()
    products(lambda at: x_all[at], uw, 0, ht)
    tp_scatter(ht, tp_h, th_s, th_r)
    gc.forward()
    tp_scatter_wait(tp_h, th_s, th_r)

    @pl.loop(0, n_fs)
    def _(i):
        h_all[i, mine, :] = tp_total(ht, tp_h, i).astype(BF16)

    tp_gather(lambda at: h_all.at[:, at, :], ah_s, ah_r)
    for k in range(1, n_fs):
        g = fs_peer(k)
        go(send(h_all.at[g, mine, :], hn.at[mine, unit(f)], hna_s.at[k], hna_r.at[f], fs=g))
    hn[mine, unit(f)] = h_all[f, mine, :]
    tp_gather_wait(lambda at: h_all.at[:, at, :], ah_s, ah_r)
    products(lambda at: relu_squared(h_all[at]), dw, 0, ot)
    sum_o.start()
    gp.start()

    gc.finish()
    products(lambda at: c_all[at], dw, 1, bt)
    tp_scatter(bt, tp_b, tb_s, tb_r)
    for k in range(1, n_fs):
        g = fs_peer(k)
        landed(hp_all.at[g, mine, :], hps_s.at[0], hps_r.at[g], fs=g)
    tp_gather(lambda at: hp_all.at[:, at, :], hpt_s, hpt_r)
    tp_scatter_wait(tp_b, tb_s, tb_r)

    @pl.loop(0, n_fs)
    def _(i):
        slope = jnp.maximum(hp_all[i, mine, :].astype(F32), 0.0)
        hg_all[i, mine, :] = (tp_total(bt, tp_b, i) * 2.0 * slope).astype(BF16)

    tp_gather(lambda at: hg_all.at[:, at, :], ab_s, ab_r)
    tp_gather_wait(lambda at: hg_all.at[:, at, :], ab_s, ab_r)
    products(lambda at: hg_all[at], uw, 1, it)
    sum_i.start()
    sum_o.spread()
    sum_o.relay()
    gp.start_mate()
    gp.relay()
    gp.forward()

    tp_gather_wait(lambda at: hp_all.at[:, at, :], hpt_s, hpt_r)
    load_ua.wait()
    load_da.wait()

    def accumulate(left_of, right, total):
        high = min(total.shape[0], 256)

        @pl.loop(0, total.shape[0] // high)
        def _(i):
            at = pl.ds(pl.multiple_of(i * high, high), high)
            total[at, :] += contract(left_of(at), right(), 0, 0)

    def flat(values):
        return values.reshape(n_fs * rows, values.shape[-1])

    def accumulate_up(side):
        blocks = [k * PAIR + side for k in range(n_z)]
        accumulate(
            lambda at: jnp.concatenate([p_all[b, :, at] for b in blocks]),
            lambda: jnp.concatenate([hg_all[b] for b in blocks]),
            ua,
        )

    accumulate(lambda at: flat(relu_squared(hp_all[:, :, at])), lambda: flat(c_all[...]), da)
    accumulate_up(y)
    sum_i.spread()
    sum_i.relay()

    for k in range(1, n_fs):
        g = fs_peer(k)
        landed(hn.at[mine, unit(g)], hna_s.at[0], hna_r.at[g], fs=g)
    tp_gather(lambda at: hn.at[at, :], hnt_s, hnt_r)
    sum_o.finish(out)
    gp.finish()
    accumulate_up(1 - y)
    sum_i.finish(ig)
    tp_gather_wait(lambda at: hn.at[at, :], hnt_s, hnt_r)
    for copy in sent:
        copy.wait_send()


def local(n_fs, n_tp, xn, xp, hp, ct, uw, dw, ua, da):
    rows, depth = xn.shape
    width = dw.shape[0]
    n_z = n_fs // PAIR
    part = rows // n_tp
    dma = pltpu.SemaphoreType.DMA

    def held(*shape, dtype=BF16):
        return pltpu.VMEM(shape, dtype)

    def tokens(columns):
        return held(n_fs, rows, columns)

    vmem, hbm = pl.BlockSpec(memory_space=pltpu.VMEM), pl.BlockSpec(memory_space=pltpu.HBM)
    fs_sem, tp_sem, z_sem = dma((n_fs,)), dma((n_tp,)), dma((n_z,))
    return pl.pallas_call(
        functools.partial(kernel, n_fs, n_tp),
        out_shape=(
            pltpu.VMEM(xn.shape, BF16),
            pltpu.VMEM(hp.shape, BF16),
            pltpu.VMEM(xp.shape, BF16),
            pltpu.VMEM(ua.shape, F32),
            pltpu.VMEM(da.shape, F32),
        ),
        in_specs=[hbm] * 8,
        out_specs=(vmem,) * 5,
        scratch_shapes=[
            held(rows, depth), held(rows, depth), held(*hp.shape), held(rows, depth),
            held(*uw.shape), held(*dw.shape),
            tokens(depth), tokens(depth), tokens(depth),
            tokens(width), tokens(width), tokens(width),
            tokens(width), tokens(width),
            held(n_tp, n_fs, part, width), held(n_tp, n_fs, part, width),
            tokens(depth), tokens(depth),
            held(n_z, rows, depth), held(n_z, rows, depth),
            held(n_z, rows, depth), held(n_z, rows, depth),
            held(n_z // 2, rows, depth), held(n_z // 2, rows, depth),
            held(n_z // 2 + 1, rows, depth), held(n_z // 2 + 1, rows, depth),
            fs_sem, fs_sem, fs_sem, fs_sem, fs_sem, fs_sem, fs_sem, fs_sem, tp_sem, tp_sem,
            tp_sem, tp_sem, tp_sem, tp_sem, tp_sem, tp_sem, tp_sem, tp_sem,
            fs_sem, fs_sem, tp_sem, tp_sem,
            z_sem, z_sem, z_sem, z_sem, z_sem, z_sem, z_sem, z_sem,
            z_sem, z_sem, z_sem, z_sem,
            dma((8,)),
        ],
        compiler_params=pltpu.CompilerParams(
            collective_id=0, has_side_effects=True, vmem_limit_bytes=52 * 1024 * 1024
        ),
    )(xn, xp, hp, ct, uw, dw, ua, da)


def solution(mesh):
    return jax.shard_map(
        functools.partial(local, mesh.shape["fs"], mesh.shape["tp"]),
        mesh=mesh,
        in_specs=(
            P(("rep", "fs"), "tp"),
            P(("rep", "fs"), "tp"),
            P(("rep", "fs"), None),
            P(("rep", "fs"), "tp"),
            P("tp", "fs"),
            P("fs", "tp"),
            P(("rep", "tp"), "fs"),
            P(("rep", "fs"), "tp"),
        ),
        out_specs=(
            P(("rep", "fs"), "tp"),
            P(("rep", "fs"), None),
            P(("rep", "fs"), "tp"),
            P(("rep", "tp"), "fs"),
            P(("rep", "fs"), "tp"),
        ),
        check_vma=False,
    )
```

```python
import functools

import jax
import jax.numpy as jnp
from jax import lax
from jax.experimental import pallas as pl
from jax.experimental.pallas import tpu as pltpu
from jax.sharding import PartitionSpec as P

F32, BF16 = jnp.float32, jnp.bfloat16
PAIR = 2


def relu_squared(values):
    return jnp.square(jnp.maximum(values.astype(F32), 0.0)).astype(BF16)


def contract(left, right, left_dim, right_dim):
    return lax.dot_general(
        left, right, (((left_dim,), (right_dim,)), ((), ())), preferred_element_type=F32
    )


def send(src, dst, send_sem, recv_sem, **target):
    return pltpu.make_async_remote_copy(
        src_ref=src, dst_ref=dst, send_sem=send_sem, recv_sem=recv_sem,
        device_id=target, device_id_type=pl.DeviceIdType.MESH,
    )


def kernel(
    n_fs, n_tp,
    xn_hbm, xp_hbm, hp_hbm, ct_hbm, uw_hbm, dw_hbm, ua_hbm, da_hbm,
    out, hn, ig, ua, da,
    xn, xp, hp, ct, uw, dw,
    x_all, c_all, p_all, hp_all, h_all, hg_all,
    ht, bt, tp_h, tp_b, ot, it, ry_o, ry_i, ps_o, ps_i, rr_o, rr_i, rz_o, rz_i,
    x_s, x_r, c_s, c_r, p_s, p_r, hps_s, hps_r, hpt_s, hpt_r,
    th_s, th_r, tb_s, tb_r, ah_s, ah_r, ab_s, ab_r, hna_s, hna_r, hnt_s, hnt_r,
    yo_s, yo_r, zo_s, zo_r, yi_s, yi_r, zi_s, zi_r, ro_s, ro_r, ri_s, ri_r, load_s,
):
    f, t = lax.axis_index("fs"), lax.axis_index("tp")
    n_z = n_fs // PAIR
    z, y = f // PAIR, lax.rem(f, PAIR)
    mate = z * PAIR + (1 - y)
    hs = n_z // 2
    low, at_half = z // hs * hs, lax.rem(z, hs)
    rows, width = xn.shape[0], dw.shape[0]
    part = rows // n_tp
    mine = pl.ds(pl.multiple_of(t * part, part), part)

    def z_peer(k):
        return lax.rem(z + k, n_z)

    def cross_of(zz):
        return lax.rem(zz + hs, n_z)

    cross = cross_of(z)

    def half_peer(k):
        return low + lax.rem(at_half + k, hs)

    def fs_peer(k):
        return lax.rem(f + k, n_fs)

    def tp_peer(k):
        return lax.rem(t + k, n_tp)

    def part_of(p):
        return pl.ds(pl.multiple_of(p * part, part), part)

    def unit(g):
        return pl.ds(pl.multiple_of(g * width, width), width)

    sent = []

    def go(copy):
        copy.start()
        sent.append(copy)

    def landed(dst, send_sem, recv_sem, **target):
        send(dst, dst, send_sem, recv_sem, **target).wait_recv()

    class Gather:
        def __init__(self, own, whole, ss, rs):
            self.own, self.whole, self.ss, self.rs, self.used = own, whole, ss, rs, 0

        def put(self, src, block, g):
            go(send(src, self.whole.at[block], self.ss.at[self.used], self.rs.at[block], fs=g))
            self.used += 1

        def wait(self, block):
            landed(self.whole.at[block], self.ss.at[0], self.rs.at[block], fs=mate)

        def start(self):
            self.put(self.own, f, cross * PAIR + y)
            for k in range(1, hs):
                self.put(self.own, f, half_peer(k) * PAIR + y)
            self.whole[f] = self.own[...]

        def start_mate(self):
            self.put(self.own, f, mate)

        def relay(self):
            block = cross * PAIR + y
            self.wait(block)
            for k in range(1, hs):
                self.put(self.whole.at[block], block, half_peer(k) * PAIR + y)
            self.put(self.whole.at[block], block, mate)

        def forward(self):
            for move in (lambda p: p, cross_of):
                for k in range(1, hs):
                    block = move(half_peer(k)) * PAIR + y
                    self.wait(block)
                    self.put(self.whole.at[block], block, mate)

        def forward_wide(self):
            self.wait(mate)
            for k in range(1, hs):
                self.put(self.whole.at[mate], mate, half_peer(k) * PAIR + y)
            for k in range(1, hs):
                self.wait(half_peer(k) * PAIR + y)
            for k in range(1, hs):
                block = cross_of(half_peer(k)) * PAIR + y
                self.wait(block)
                self.put(self.whole.at[block], block, mate)

        def finish(self, first=0):
            for k in range(first, n_z):
                self.wait(z_peer(k) * PAIR + (1 - y))

    def tp_scatter(terms, held, ss, rs):
        for k in range(1, n_tp):
            p = tp_peer(k)
            go(send(terms.at[:, part_of(p), :], held.at[t], ss.at[k], rs.at[t], tp=p))

    def tp_scatter_wait(held, ss, rs):
        for k in range(1, n_tp):
            p = tp_peer(k)
            landed(held.at[p], ss.at[0], rs.at[p], tp=p)

    def tp_gather(view, ss, rs):
        for k in range(1, n_tp):
            go(send(view(mine), view(mine), ss.at[k], rs.at[t], tp=tp_peer(k)))

    def tp_gather_wait(view, ss, rs):
        for k in range(1, n_tp):
            p = tp_peer(k)
            landed(view(part_of(p)), ss.at[0], rs.at[p], tp=p)

    def tp_total(terms, held, i):
        total = terms[i, mine, :].astype(F32)
        for k in range(1, n_tp):
            total = total + held[tp_peer(k), i].astype(F32)
        return total

    def products(left_of, right, right_dim, terms):
        @pl.loop(0, n_fs // PAIR)
        def _(i):
            left = left_of(pl.ds(i * PAIR, PAIR))
            left = left.reshape(PAIR * rows, left.shape[-1])
            total = contract(left, right[...], 1, right_dim).astype(BF16)
            terms[pl.ds(i * PAIR, PAIR)] = total.reshape(PAIR, rows, total.shape[-1])

    class Scatter:
        def __init__(self, terms, ry, ps, rr, rz, sems):
            self.terms, self.ry, self.ps, self.rr, self.rz = terms, ry, ps, rr, rz
            self.ys, self.yr, self.rs, self.rrecv, self.zs, self.zr = sems

        def start(self):
            order = [cross_of(half_peer(k)) for k in range(1, hs)] + [cross]
            order += [half_peer(k) for k in range(1, hs)] + [z]
            for k, zz in enumerate(order):
                block = self.terms.at[zz * PAIR + (1 - y)]
                go(send(block, self.ry.at[zz], self.ys.at[k], self.yr.at[zz], fs=mate))

        def pair(self, zz):
            landed(self.ry.at[zz], self.ys.at[0], self.yr.at[zz], fs=mate)
            return self.terms[zz * PAIR + y].astype(F32) + self.ry[zz].astype(F32)

        def spread(self):
            for k in range(1, hs):
                p = half_peer(k)
                zz = cross_of(p)
                self.ps[zz] = self.pair(zz).astype(BF16)
                slot, sem = self.rr.at[at_half], self.rrecv.at[at_half]
                go(send(self.ps.at[zz], slot, self.rs.at[k], sem, fs=p * PAIR + y))

        def relay(self):
            total = self.pair(cross)
            for k in range(1, hs):
                p = half_peer(k)
                w = p - low
                landed(self.rr.at[w], self.rs.at[0], self.rrecv.at[w], fs=p * PAIR + y)
                total = total + self.rr[w].astype(F32)
            self.ps[cross] = total.astype(BF16)
            go(send(
                self.ps.at[cross], self.rz.at[hs], self.zs.at[0], self.zr.at[hs],
                fs=cross * PAIR + y,
            ))
            for k in range(1, hs):
                p = half_peer(k)
                self.ps[p] = self.pair(p).astype(BF16)
                slot, sem = self.rz.at[at_half], self.zr.at[at_half]
                go(send(self.ps.at[p], slot, self.zs.at[k], sem, fs=p * PAIR + y))

        def finish(self, result):
            total = self.pair(z)
            for k in range(1, hs):
                p = half_peer(k)
                w = p - low
                landed(self.rz.at[w], self.zs.at[0], self.zr.at[w], fs=p * PAIR + y)
                total = total + self.rz[w].astype(F32)
            landed(self.rz.at[hs], self.zs.at[0], self.zr.at[hs], fs=cross * PAIR + y)
            result[...] = (total + self.rz[hs].astype(F32)).astype(BF16)

    def load(k, src, dst):
        copy = pltpu.make_async_copy(src, dst, load_s.at[k])
        copy.start()
        return copy

    load_xn, load_ct, load_xp = load(0, xn_hbm, xn), load(1, ct_hbm, ct), load(2, xp_hbm, xp)
    load_hp, load_uw, load_dw = load(3, hp_hbm, hp), load(4, uw_hbm, uw), load(5, dw_hbm, dw)
    load_ua, load_da = load(6, ua_hbm, ua), load(7, da_hbm, da)

    barrier = pltpu.get_barrier_semaphore()
    for k in range(1, n_fs):
        pl.semaphore_signal(
            barrier, inc=1, device_id={"fs": fs_peer(k)}, device_id_type=pl.DeviceIdType.MESH
        )
    for k in range(1, n_tp):
        pl.semaphore_signal(
            barrier, inc=1, device_id={"tp": tp_peer(k)}, device_id_type=pl.DeviceIdType.MESH
        )
    pl.semaphore_wait(barrier, n_fs + n_tp - 2)

    gx = Gather(xn, x_all, x_s, x_r)
    gc = Gather(ct, c_all, c_s, c_r)
    gp = Gather(xp, p_all, p_s, p_r)
    sum_o = Scatter(ot, ry_o, ps_o, rr_o, rz_o, (yo_s, yo_r, ro_s, ro_r, zo_s, zo_r))
    sum_i = Scatter(it, ry_i, ps_i, rr_i, rz_i, (yi_s, yi_r, ri_s, ri_r, zi_s, zi_r))

    load_xn.wait()
    gx.start()
    gx.start_mate()
    load_ct.wait()
    gc.start_mate()
    load_xp.wait()
    load_hp.wait()
    hp_all[f, mine, :] = hp[mine, unit(f)]
    load_uw.wait()
    load_dw.wait()
    gx.relay()
    gp.start_mate()
    gc.start()
    gx.forward()
    gc.relay()
    for k in range(1, n_fs):
        g = fs_peer(k)
        go(send(hp.at[mine, unit(g)], hp_all.at[f, mine, :], hps_s.at[k], hps_r.at[f], fs=g))

    gx.finish()
    products(lambda at: x_all[at], uw, 0, ht)
    tp_scatter(ht, tp_h, th_s, th_r)
    gc.forward()
    tp_scatter_wait(tp_h, th_s, th_r)

    @pl.loop(0, n_fs)
    def _(i):
        h_all[i, mine, :] = tp_total(ht, tp_h, i).astype(BF16)

    tp_gather(lambda at: h_all.at[:, at, :], ah_s, ah_r)
    for k in range(1, n_fs):
        g = fs_peer(k)
        go(send(h_all.at[g, mine, :], hn.at[mine, unit(f)], hna_s.at[k], hna_r.at[f], fs=g))
    hn[mine, unit(f)] = h_all[f, mine, :]
    tp_gather_wait(lambda at: h_all.at[:, at, :], ah_s, ah_r)
    products(lambda at: relu_squared(h_all[at]), dw, 0, ot)
    sum_o.start()
    gp.start()

    gc.finish()
    products(lambda at: c_all[at], dw, 1, bt)
    tp_scatter(bt, tp_b, tb_s, tb_r)
    for k in range(1, n_fs):
        g = fs_peer(k)
        landed(hp_all.at[g, mine, :], hps_s.at[0], hps_r.at[g], fs=g)
    tp_gather(lambda at: hp_all.at[:, at, :], hpt_s, hpt_r)
    tp_scatter_wait(tp_b, tb_s, tb_r)

    @pl.loop(0, n_fs)
    def _(i):
        slope = jnp.maximum(hp_all[i, mine, :].astype(F32), 0.0)
        hg_all[i, mine, :] = (tp_total(bt, tp_b, i) * 2.0 * slope).astype(BF16)

    tp_gather(lambda at: hg_all.at[:, at, :], ab_s, ab_r)
    tp_gather_wait(lambda at: hg_all.at[:, at, :], ab_s, ab_r)
    products(lambda at: hg_all[at], uw, 1, it)
    sum_i.start()
    sum_o.spread()
    sum_o.relay()
    gp.relay()
    gp.forward_wide()

    tp_gather_wait(lambda at: hp_all.at[:, at, :], hpt_s, hpt_r)
    load_ua.wait()
    load_da.wait()

    def accumulate(left_of, right, total):
        high = min(total.shape[0], 256)

        @pl.loop(0, total.shape[0] // high)
        def _(i):
            at = pl.ds(pl.multiple_of(i * high, high), high)
            total[at, :] += contract(left_of(at), right(), 0, 0)

    def flat(values):
        return values.reshape(n_fs * rows, values.shape[-1])

    def accumulate_up(side):
        blocks = [k * PAIR + side for k in range(n_z)]
        accumulate(
            lambda at: jnp.concatenate([p_all[b, :, at] for b in blocks]),
            lambda: jnp.concatenate([hg_all[b] for b in blocks]),
            ua,
        )

    accumulate(lambda at: flat(relu_squared(hp_all[:, :, at])), lambda: flat(c_all[...]), da)
    accumulate_up(y)
    sum_i.spread()
    sum_i.relay()

    for k in range(1, n_fs):
        g = fs_peer(k)
        landed(hn.at[mine, unit(g)], hna_s.at[0], hna_r.at[g], fs=g)
    tp_gather(lambda at: hn.at[at, :], hnt_s, hnt_r)
    sum_o.finish(out)
    gp.finish(1)
    accumulate_up(1 - y)
    sum_i.finish(ig)
    tp_gather_wait(lambda at: hn.at[at, :], hnt_s, hnt_r)
    for copy in sent:
        copy.wait_send()


def write_out(*refs):
    sems = refs[-1]
    copies = [pltpu.make_async_copy(refs[k], refs[5 + k], sems.at[k]) for k in (3, 4, 1, 0, 2)]
    for copy in copies:
        copy.start()
    for copy in copies:
        copy.wait()


def local(n_fs, n_tp, xn, xp, hp, ct, uw, dw, ua, da):
    rows, depth = xn.shape
    width = dw.shape[0]
    n_z = n_fs // PAIR
    part = rows // n_tp
    dma = pltpu.SemaphoreType.DMA

    def held(*shape, dtype=BF16):
        return pltpu.VMEM(shape, dtype)

    def tokens(columns):
        return held(n_fs, rows, columns)

    vmem, hbm = pl.BlockSpec(memory_space=pltpu.VMEM), pl.BlockSpec(memory_space=pltpu.HBM)
    fs_sem, tp_sem, z_sem = dma((n_fs,)), dma((n_tp,)), dma((n_z,))
    results = pl.pallas_call(
        functools.partial(kernel, n_fs, n_tp),
        out_shape=(
            pltpu.VMEM(xn.shape, BF16),
            pltpu.VMEM(hp.shape, BF16),
            pltpu.VMEM(xp.shape, BF16),
            pltpu.VMEM(ua.shape, F32),
            pltpu.VMEM(da.shape, F32),
        ),
        in_specs=[hbm] * 8,
        out_specs=(vmem,) * 5,
        scratch_shapes=[
            held(rows, depth), held(rows, depth), held(*hp.shape), held(rows, depth),
            held(*uw.shape), held(*dw.shape),
            tokens(depth), tokens(depth), tokens(depth),
            tokens(width), tokens(width), tokens(width),
            tokens(width), tokens(width),
            held(n_tp, n_fs, part, width), held(n_tp, n_fs, part, width),
            tokens(depth), tokens(depth),
            held(n_z, rows, depth), held(n_z, rows, depth),
            held(n_z, rows, depth), held(n_z, rows, depth),
            held(n_z // 2, rows, depth), held(n_z // 2, rows, depth),
            held(n_z // 2 + 1, rows, depth), held(n_z // 2 + 1, rows, depth),
            fs_sem, fs_sem, fs_sem, fs_sem, fs_sem, fs_sem, fs_sem, fs_sem, tp_sem, tp_sem,
            tp_sem, tp_sem, tp_sem, tp_sem, tp_sem, tp_sem, tp_sem, tp_sem,
            fs_sem, fs_sem, tp_sem, tp_sem,
            z_sem, z_sem, z_sem, z_sem, z_sem, z_sem, z_sem, z_sem,
            z_sem, z_sem, z_sem, z_sem,
            dma((8,)),
        ],
        compiler_params=pltpu.CompilerParams(
            collective_id=0, has_side_effects=True, vmem_limit_bytes=52 * 1024 * 1024
        ),
    )(xn, xp, hp, ct, uw, dw, ua, da)
    return pl.pallas_call(
        write_out,
        out_shape=tuple(jax.ShapeDtypeStruct(r.shape, r.dtype) for r in results),
        in_specs=[pl.BlockSpec(memory_space=pl.ANY)] * 5,
        out_specs=(hbm,) * 5,
        scratch_shapes=[dma((5,))],
        compiler_params=pltpu.CompilerParams(vmem_limit_bytes=1024 * 1024),
    )(*results)


def solution(mesh):
    return jax.shard_map(
        functools.partial(local, mesh.shape["fs"], mesh.shape["tp"]),
        mesh=mesh,
        in_specs=(
            P(("rep", "fs"), "tp"),
            P(("rep", "fs"), "tp"),
            P(("rep", "fs"), None),
            P(("rep", "fs"), "tp"),
            P("tp", "fs"),
            P("fs", "tp"),
            P(("rep", "tp"), "fs"),
            P(("rep", "fs"), "tp"),
        ),
        out_specs=(
            P(("rep", "fs"), "tp"),
            P(("rep", "fs"), None),
            P(("rep", "fs"), "tp"),
            P(("rep", "tp"), "fs"),
            P(("rep", "fs"), "tp"),
        ),
        check_vma=False,
    )
```
